32 devices in a mesh: ep: 8 (over z, x), tp: 4 (over y, core).
Axes of the slice: x: 2, y: 2, z: 4, core: 2. Of those that a mesh axis runs over, the one named last changes fastest.
Arguments:
- tokens: bfloat16 [256, 2048], P('ep'), may hold values from -6 to 6
- norm_gain: float32 [2048], replicated, may hold values from 0.1 to 1.9
- norm_bias: float32 [2048], replicated, may hold values from -3 to 3
- routes: int32 [256, 4], P('ep'), may hold values from 0 to 7, all different within a row; in each aligned block of 32 rows (0 to 31, 32 to 63, ...) at most 32 rows name the same one
- route_weights: float32 [256, 4], P('ep'), may hold values from 0.2 to 1
- gate_w: bfloat16 [8, 2048, 4096], P('ep', None, 'tp'), may hold values from -0.125 to 0.125
- up_w: bfloat16 [8, 2048, 4096], P('ep', None, 'tp'), may hold values from -0.125 to 0.125
- down_w: bfloat16 [8, 4096, 2048], P('ep', 'tp'), may hold values from -0.09375 to 0.09375
Outputs:
- mixed: bfloat16 [256, 2048], P('ep', 'tp')
The draws below stay inside these ranges and needn't reach their ends.
Inputs may be any that keep to these rules, and one draw needn't show every extreme that they name: `routes`: the 4 experts of a token differ; the rows of one index of ep name no expert more than 32 times, and in every draw some index of ep names some expert exactly 32 times.
All inputs are finite; a program needn't handle non-finite values.
Results may differ from the reference program's by a relative error of at most 0.017.
Values may be sent and summed in bfloat16 or wider, within the bound.
A program may use at most 64 MiB of HBM per device.

```python
import math
import jax
import jax.numpy as jnp
import numpy as np
from jax import lax

D = 2048
FF = 4096
TOPK = 4
TOK_DEV = 32
EXPERTS = 8
CAP = 32
TOKENS = 256
N_TP = 4


def block_scale(rng, dims, shards, smallest, top_value):
    def one(position, parts):
        heights = jax.random.uniform(jax.random.fold_in(jax.random.fold_in(rng, 6), position), (parts,), jnp.float32, smallest / len(shards), top_value / len(shards))
        return jnp.repeat(jnp.exp(heights), dims[position] // parts).reshape((-1,) + (1,) * (len(dims) - position - 1))

    level = one(*shards[0])
    for cut in shards[1:]:
        level = level * one(*cut)
    return level


def deal_out(own_key, own, number, rows, number_of, top, bound, lean):
    sequence = jax.random.permutation(own_key, number_of)
    crowded, common = shares(number_of, rows * top, bound, lean, True), shares(number_of, rows * top, bound, lean, False)
    places = jnp.arange(number_of)

    def named(tallies, turn):
        used = int((tallies > 0).sum())
        fixed = max(1, used // 4)
        moved = fixed + (places - fixed + turn * (used - fixed)) % max(1, number_of - fixed)
        return jnp.zeros((number_of,), jnp.int32).at[sequence[jnp.where(places < fixed, places, moved)]].set(jnp.asarray(tallies, jnp.int32))

    tallies = jnp.where(number % 4 == 0, named(crowded, number // 4), named(common, number - number // 4 - 1))
    mixed = jax.random.permutation(jax.random.fold_in(own, 3), number_of)
    donor, sink = mixed[0:number_of // 2 * 2:2], mixed[1:number_of // 2 * 2:2]
    slack = jnp.minimum(tallies[donor] - 1, bound - tallies[sink]) // 2
    slack = jnp.where((donor == sequence[0]) | (sink == sequence[0]) | (tallies[sink] == 0), 0, jnp.maximum(slack, 0))
    moved = jax.random.randint(jax.random.fold_in(own, 4), (number_of // 2,), 0, 1 << 20) % (slack + 1)
    tallies = tallies.at[donor].add(-moved).at[sink].add(moved)
    labels = jnp.searchsorted(jnp.cumsum(tallies), jnp.arange(rows * top), side="right").astype(jnp.int32)
    listing = labels.reshape(top, rows).T
    listing = listing[jax.random.permutation(jax.random.fold_in(own, 1), rows)]
    turn = jax.random.randint(jax.random.fold_in(own, 2), (rows, 1), 0, top)
    return jnp.take_along_axis(listing, (jnp.arange(top)[None, :] + turn) % top, axis=1)


def shares(count, total, reach, slope, full):
    portions = [(1 << 20) // math.isqrt(rank ** slope) + 1 for rank in range(1, count + 1)]
    largest = reach if full else min(reach, max(-(-total // count), total * portions[0] // sum(portions)))
    least = 1 if total - largest >= count - 1 else 0
    counts, rest = [largest] + [least] * (count - 1), total - largest - least * (count - 1)
    while rest > 0:
        candidates = [i for i in range(1, count) if counts[i] < largest] or [i for i in range(1, count) if counts[i] < reach]
        pool, budget = sum([portions[i] for i in candidates]), rest
        for i in candidates:
            more = min(reach - counts[i], max(1, budget * portions[i] // pool), rest)
            counts[i] = counts[i] + more
            rest = rest - more
    return np.array(counts)


def scatter_about(own_key, shape, spread, most, shards=(), held_as=jnp.bfloat16):
    level = block_scale(own_key, shape, shards, -0.22, 0.18) if shards else 1.0
    drawn = jax.random.normal(own_key, shape, jnp.float32) * spread * level
    return jnp.minimum(jnp.maximum(drawn, -most), most).astype(held_as)


def setup_inputs(seed: int = 0) -> dict:
    splits = jax.random.split(jax.random.key(seed), 9)
    tokens = scatter_about(splits[0], (TOKENS, D), 1.0, 6.0, ((0, 8),))
    norm_gain = jnp.clip(1.0 + 0.18 * jax.random.normal(splits[1], (D,), jnp.float32), 0.1, 1.9)
    norm_bias = scatter_about(splits[2], (D,), 0.5, 3.0, (), jnp.float32)
    routes_keys = jax.random.split(jax.random.fold_in(splits[3], 1), TOKENS // TOK_DEV)
    routes_turns = jax.random.permutation(jax.random.fold_in(splits[3], 3), TOKENS // TOK_DEV)
    routes = jax.vmap(lambda own, number: deal_out(jax.random.fold_in(splits[3], 2), own, number, TOK_DEV, EXPERTS, TOPK, CAP, 2))(routes_keys, routes_turns).reshape((TOKENS, TOPK))
    route_weights = jnp.clip(0.2 + 0.8 * jax.random.uniform(splits[4], (TOKENS, TOPK), jnp.float32) ** block_scale(splits[4], (TOKENS, TOPK), ((0, 8),), -0.2, 0.2), 0.2, 1.0)
    gate_w = scatter_about(splits[5], (EXPERTS, D, FF), D ** -0.5, 0.125, ((0, 8), (2, 4)))
    up_w = scatter_about(splits[6], (EXPERTS, D, FF), D ** -0.5, 0.125, ((0, 8), (2, 4)))
    down_w = scatter_about(splits[7], (EXPERTS, FF, D), FF ** -0.5, 0.09375, ((0, 8), (1, 4)))
    return {"tokens": tokens, "norm_gain": norm_gain, "norm_bias": norm_bias, "routes": routes, "route_weights": route_weights, "gate_w": gate_w, "up_w": up_w, "down_w": down_w}


def layer_norm(tokens, norm_gain, norm_bias):
    values = tokens.astype(jnp.float32)
    centred = values - lax.optimization_barrier(jnp.mean(values, axis=-1, keepdims=True))
    variance = lax.optimization_barrier(jnp.mean(centred * centred, axis=-1, keepdims=True))
    return (centred * lax.rsqrt(variance + 1e-05) * norm_gain + norm_bias).astype(jnp.bfloat16)

def reference(tokens, norm_gain, norm_bias, routes, route_weights, gate_w, up_w, down_w):
    normed = layer_norm(tokens, norm_gain, norm_bias)
    groups = N_TP
    width = down_w.shape[2]
    hidden_units = down_w.shape[1]

    def one_expert(weights):
        gate_one, up_one, down_one = weights
        gate = jnp.dot(normed, gate_one, preferred_element_type=jnp.float32)
        up = jnp.dot(normed, up_one, preferred_element_type=jnp.float32)
        hidden = (jax.nn.silu(gate) * up).astype(jnp.bfloat16)
        hidden_groups = hidden.reshape(hidden.shape[0], groups, hidden_units // groups).astype(jnp.float32)
        down_groups = down_one.reshape(groups, hidden_units // groups, width).astype(jnp.float32)
        partial_sums = jnp.einsum('tgf,gfd->gtd', hidden_groups, down_groups).astype(jnp.bfloat16)
        return lax.optimization_barrier(jnp.sum(partial_sums.astype(jnp.float32), axis=0)).astype(jnp.bfloat16)
    expert_out = lax.map(one_expert, (gate_w, up_w, down_w))
    rows = jnp.arange(tokens.shape[0], dtype=jnp.int32)[:, None]
    chosen = expert_out[routes, rows].astype(jnp.float32)
    return lax.optimization_barrier(jnp.sum(route_weights[:, :, None] * chosen, axis=1)).astype(jnp.bfloat16)
```

```python
import functools

import jax
import jax.numpy as jnp
from jax import lax
from jax.experimental import pallas as pl
from jax.experimental.pallas import tpu as pltpu
from jax.sharding import PartitionSpec as P

MESH = pl.DeviceIdType.MESH
LANES = 128


def offsets(count):
    return sorted(range(1, count), key=lambda o: (abs(2 * o - count), o))


def kernel(
    dims, tokens_hbm, gain_hbm, bias_hbm, routes_hbm, weights_hbm, gate_hbm, up_hbm, down_hbm, out_ref,
    tokens, gain, bias, routes, weights,
    buf, gate_v, up_v, down_v, hidden, partial, summed, kept_y, kept_x, from_core, from_y, from_x, from_z,
    input_sem, weight_sem, ag_send, ag_recv, core_send, core_recv, y_send, y_recv, x_send, x_recv, z_send, z_recv,
):
    nz, nx, ny, nc = dims
    f32, bf16 = jnp.float32, jnp.bfloat16
    ep, tp = lax.axis_index("ep"), lax.axis_index("tp")
    z, x = ep // nx, lax.rem(ep, nx)
    y, c = tp // nc, lax.rem(tp, nc)
    other = lax.rem(c + 1, nc)
    groups = 2 if nz % 2 == 0 else 1
    span = nz // groups
    near = (z // span) * span
    lower = z < span

    def along(value, step, count):
        return lax.rem(value + step, count)

    def at(z_index, x_index):
        return (z_index * nx + x_index, tp)

    def x_at(step):
        return along(x, step, nx)

    def at_y(step):
        return (ep, along(y, step, ny) * nc + c)

    partner = (ep, y * nc + other)

    def base(group):
        return near if group == 0 else span - near

    def z_of(group, k):
        if group == 0:
            return near + along(z - near, k, span)
        return jnp.where(lower, span + k, span - 1 - k)

    def chunks(group):
        return list(range(1, span)) + [0] if group == 0 else list(reversed(range(span)))

    others = [z_of(0, k) for k in range(1, span)]
    far = [z_of(1, k) for k in range(span)] if groups == 2 else []

    barrier = pltpu.get_barrier_semaphore()
    greeted = [partner]
    greeted += [at(i, x) for i in far + others]
    greeted += [at(z, x_at(s)) for s in offsets(nx)]
    greeted += [at_y(s) for s in offsets(ny)]
    for target in greeted:
        pl.semaphore_signal(barrier, inc=1, device_id=target, device_id_type=MESH)

    inputs = []
    for i, (hbm, vmem) in enumerate(
        (
            (tokens_hbm, tokens),
            (gain_hbm, gain),
            (bias_hbm, bias),
            (routes_hbm, routes),
            (weights_hbm, weights),
        )
    ):
        load = pltpu.make_async_copy(hbm, vmem, input_sem.at[i])
        load.start()
        inputs.append(load)

    for load in inputs:
        load.wait()
    tiles, tile = gate_v.shape[0], gate_v.shape[2]
    out_tiles, out_tile = down_v.shape[0], down_v.shape[2]
    loads = []
    for i in range(tiles):
        for which, (hbm, vmem) in enumerate(((gate_hbm, gate_v), (up_hbm, up_v))):
            load = pltpu.make_async_copy(
                hbm.at[0, :, pl.ds(i * tile, tile)], vmem.at[i], weight_sem.at[which, i]
            )
            load.start()
            loads.append(load)
    for i in range(out_tiles):
        load = pltpu.make_async_copy(
            down_hbm.at[0, :, pl.ds(i * out_tile, out_tile)], down_v.at[i], weight_sem.at[2, i]
        )
        load.start()
        loads.append(load)

    width = tokens.shape[1]
    half = width // nc
    values = tokens[...].astype(f32)
    centred = values - jnp.mean(values, axis=-1, keepdims=True)
    variance = jnp.mean(centred * centred, axis=-1, keepdims=True)
    normed = (centred * lax.rsqrt(variance + 1e-05) * gain[...] + bias[...]).astype(bf16)
    rows = tokens.shape[0]
    expert = lax.broadcasted_iota(jnp.int32, (LANES, rows), 0)
    mix = jnp.zeros((LANES, rows), f32)
    for k in range(routes.shape[0]):
        mix = mix + jnp.where(routes[k : k + 1, :] == expert, weights[k : k + 1, :], 0.0)
    mix = mix.T
    high = mix.astype(bf16)
    low = (mix - high.astype(f32)).astype(bf16)
    for i in range(nc):
        buf[ep, i, :, 0:half] = normed[:, i * half : (i + 1) * half]
        buf[ep, i, :, half : half + LANES] = high if i == 0 else low
    pl.semaphore_wait(barrier, len(greeted))

    sent = []

    cuts = ag_recv.shape[2]
    cut_rows = rows // cuts

    def piece(source, part, cut):
        if cut is None:
            return buf.at[source, part], ag_recv.at[source, part, 0]
        at_rows = pl.ds(pl.multiple_of(cut * cut_rows, cut_rows), cut_rows)
        return buf.at[source, part, at_rows], ag_recv.at[source, part, cut]

    def forward(source, target, cut=None):
        block, sem = piece(source, c, cut)
        copy = pltpu.make_async_remote_copy(
            src_ref=block,
            dst_ref=block,
            send_sem=ag_send.at[len(sent)],
            recv_sem=sem,
            device_id=target,
            device_id_type=MESH,
        )
        copy.start()
        sent.append(copy)

    def arrived(source, part, cut=None):
        block, sem = piece(source, part, cut)
        pltpu.make_async_remote_copy(
            src_ref=block,
            dst_ref=block,
            send_sem=ag_send.at[0],
            recv_sem=sem,
            device_id=partner,
            device_id_type=MESH,
        ).wait_recv()

    mine = y if cuts > 1 else None

    def share_out(source, cut):
        if cut is not None:
            for s in offsets(ny):
                forward(source, at_y(s), cut)
        forward(source, partner, cut)

    def pass_on(i, cut=None):
        source = i * nx + x
        arrived(source, c, cut)
        for s in offsets(nx):
            forward(source, at(z, x_at(s)), cut)
        share_out(source, cut)

    def hand_over(i, cut=None):
        for s in offsets(nx):
            source = i * nx + x_at(s)
            arrived(source, c, cut)
            share_out(source, cut)

    def collect(i):
        if cuts > 1:
            for t in range(nx):
                source = i * nx + x_at(t)
                for s in offsets(ny):
                    arrived(source, c, along(y, s, ny))
                    forward(source, partner, along(y, s, ny))

    def partner_blocks(i, pieces=1):
        for s in range(nx):
            for cut in range(pieces):
                arrived(i * nx + x_at(s), other, cut if pieces > 1 else None)

    size = span * nx * rows

    def up_phase(group):
        blocks = pl.ds(base(group) * nx, span * nx)
        lanes = lax.broadcasted_iota(jnp.int32, (size, LANES), 1)
        shares = buf[blocks, 0, :, half : half + LANES].astype(f32)
        shares = (shares + buf[blocks, 1, :, half : half + LANES].astype(f32)).reshape(size, LANES)
        share = jnp.sum(jnp.where(lanes == ep, shares, 0.0), axis=1, keepdims=True)

        def step(i, carry):
            gate = jnp.zeros((size, tile), f32)
            up = jnp.zeros((size, tile), f32)
            for part in range(nc):
                block = buf[blocks, part, :, 0:half].reshape(size, half)
                depth = slice(part * half, (part + 1) * half)
                gate = gate + jnp.dot(block, gate_v[i, depth, :], preferred_element_type=f32)
                up = up + jnp.dot(block, up_v[i, depth, :], preferred_element_type=f32)
            hidden[i] = (gate / (1.0 + jnp.exp(-gate)) * up * share).astype(bf16)
            return carry

        lax.fori_loop(0, tiles, step, 0)

    def down_step(group, which):
        acc = jnp.zeros((size, out_tile), f32)
        for i in range(tiles):
            acc = acc + jnp.dot(
                hidden[i], down_v[which, i * tile : (i + 1) * tile, :], preferred_element_type=f32
            )
        partial[group, which] = acc.astype(bf16)

    core_copies, y_copies, x_copies, z_copies = {}, {}, {}, {}

    def down_phase(group):
        for s in offsets(ny) + [0]:
            column = along(y, s, ny)
            down_step(group, column * nc + other)
            copy = pltpu.make_async_remote_copy(
                src_ref=partial.at[group, column * nc + other],
                dst_ref=from_core.at[group, column],
                send_sem=core_send.at[group, column],
                recv_sem=core_recv.at[group, column],
                device_id=partner,
                device_id_type=MESH,
            )
            copy.start()
            core_copies[group, s] = copy
        for s in offsets(ny):
            down_step(group, along(y, s, ny) * nc + c)
        y_phase(group)
        down_step(group, y * nc + c)
        core_copies[group, 0].wait_recv()

    def block_rows(group, k, o):
        place = (z_of(group, k) - base(group)) * nx + x_at(o)
        return pl.ds(pl.multiple_of(place * rows, rows), rows)

    def y_phase(group):
        for s in offsets(ny):
            column = along(y, s, ny)
            core_copies[group, s].wait_recv()
            for o in offsets(nx) + [0]:
                for k in chunks(group):
                    at_rows = block_rows(group, k, o)
                    summed[s - 1, group, k, o] = (
                        partial[group, column * nc + c, at_rows, :].astype(f32)
                        + from_core[group, column, at_rows, :].astype(f32)
                    ).astype(bf16)
                    copy = pltpu.make_async_remote_copy(
                        src_ref=summed.at[s - 1, group, k, o],
                        dst_ref=from_y.at[s - 1, group, k, o],
                        send_sem=y_send.at[s - 1, group, k, o],
                        recv_sem=y_recv.at[s - 1, group, k, o],
                        device_id=at_y(s),
                        device_id_type=MESH,
                    )
                    copy.start()
                    y_copies[s, group, k, o] = copy

    def y_total(group, k, o):
        at_rows = block_rows(group, k, o)
        acc = partial[group, y * nc + c, at_rows, :].astype(f32) + from_core[group, y, at_rows, :].astype(f32)
        for s in offsets(ny):
            y_copies[s, group, k, o].wait_recv()
            acc = acc + from_y[s - 1, group, k, o].astype(f32)
        return acc

    def x_step(group, k):
        for s in offsets(nx):
            kept_y[group, k, s - 1] = y_total(group, k, s).astype(bf16)
            copy = pltpu.make_async_remote_copy(
                src_ref=kept_y.at[group, k, s - 1],
                dst_ref=from_x.at[s - 1, group, k],
                send_sem=x_send.at[s - 1, group, k],
                recv_sem=x_recv.at[s - 1, group, k],
                device_id=at(z, x_at(s)),
                device_id_type=MESH,
            )
            copy.start()
            x_copies[s, group, k] = copy

    def z_step(group, k):
        acc = y_total(group, k, 0)
        for s in offsets(nx):
            x_copies[s, group, k].wait_recv()
            acc = acc + from_x[s - 1, group, k].astype(f32)
        if group == 0 and k == 0:
            return acc
        kept_x[group, k] = acc.astype(bf16)
        copy = pltpu.make_async_remote_copy(
            src_ref=kept_x.at[group, k],
            dst_ref=from_z.at[z],
            send_sem=z_send.at[group, k],
            recv_sem=z_recv.at[z],
            device_id=at(z_of(group, k), x),
            device_id_type=MESH,
        )
        copy.start()
        z_copies[group, k] = copy

    for s in offsets(nx):
        forward(ep, at(z, x_at(s)))
    for i in others:
        forward(ep, at(i, x))
    for i in far:
        forward(ep, at(i, x), mine)
    for s in offsets(nx):
        source = z * nx + x_at(s)
        arrived(source, c)
        forward(source, partner)
    for i in others:
        pass_on(i)
    for i in far:
        pass_on(i, mine)
    for i in others:
        hand_over(i)
    for s in offsets(nx):
        arrived(z * nx + x_at(s), other)
    for i in others:
        partner_blocks(i)
    for load in loads[: 2 * tiles]:
        load.wait()
    up_phase(0)
    for i in far:
        hand_over(i, mine)
    for load in loads[2 * tiles :]:
        load.wait()
    down_phase(0)
    for i in far:
        collect(i)
    if groups == 2:
        for i in far:
            partner_blocks(i, cuts)
        up_phase(1)
    for k in chunks(0):
        x_step(0, k)
    if groups == 2:
        down_phase(1)
        for k in chunks(1):
            x_step(1, k)
    result = None
    for k in chunks(0):
        result = z_step(0, k)
    if groups == 2:
        for k in chunks(1):
            z_step(1, k)
    for i in others + far:
        pltpu.make_async_remote_copy(
            src_ref=from_z.at[i],
            dst_ref=from_z.at[i],
            send_sem=z_send.at[0, 0],
            recv_sem=z_recv.at[i],
            device_id=partner,
            device_id_type=MESH,
        ).wait_recv()
        result = result + from_z[i].astype(f32)
    out_ref[...] = result.astype(out_ref.dtype)

    for copies in (sent, core_copies.values(), y_copies.values(), x_copies.values(), z_copies.values()):
        for copy in copies:
            copy.wait_send()


def body(dims, tokens, norm_gain, norm_bias, routes, route_weights, gate_w, up_w, down_w):
    nz, nx, ny, nc = dims
    rows, width = tokens.shape
    topk = routes.shape[1]
    depth = gate_w.shape[2]
    experts, parts = nz * nx, ny * nc
    groups = 2 if nz % 2 == 0 else 1
    span = nz // groups
    size = span * nx * rows
    tile = min(256, depth)
    out_width = width // parts
    half = width // nc
    bf16, f32 = jnp.bfloat16, jnp.float32
    dma = pltpu.SemaphoreType.DMA
    hbm = pl.BlockSpec(memory_space=pl.ANY)
    y_steps, x_steps = max(ny - 1, 1), max(nx - 1, 1)
    cuts = ny if rows % (16 * ny) == 0 else 1
    ag_sends = nz + nx + (1 + 2 * cuts) * experts
    return pl.pallas_call(
        functools.partial(kernel, dims),
        out_shape=pltpu.VMEM((rows, out_width), bf16),
        in_specs=[hbm] * 8,
        out_specs=pl.BlockSpec(memory_space=pltpu.VMEM),
        scratch_shapes=[
            pltpu.VMEM((rows, width), bf16),
            pltpu.VMEM((1, width), f32),
            pltpu.VMEM((1, width), f32),
            pltpu.VMEM((topk, rows), jnp.int32),
            pltpu.VMEM((topk, rows), f32),
            pltpu.VMEM((experts, nc, rows, half + LANES), bf16),
            pltpu.VMEM((depth // tile, width, tile), bf16),
            pltpu.VMEM((depth // tile, width, tile), bf16),
            pltpu.VMEM((parts, depth, out_width), bf16),
            pltpu.VMEM((depth // tile, size, tile), bf16),
            pltpu.VMEM((groups, parts, size, out_width), bf16),
            pltpu.VMEM((y_steps, groups, span, nx, rows, out_width), bf16),
            pltpu.VMEM((groups, span, x_steps, rows, out_width), bf16),
            pltpu.VMEM((groups, span, rows, out_width), bf16),
            pltpu.VMEM((groups, ny, size, out_width), bf16),
            pltpu.VMEM((y_steps, groups, span, nx, rows, out_width), bf16),
            pltpu.VMEM((x_steps, groups, span, rows, out_width), bf16),
            pltpu.VMEM((nz, rows, out_width), bf16),
            dma((5,)),
            dma((3, max(depth // tile, parts))),
            dma((ag_sends,)),
            dma((experts, nc, cuts)),
            dma((groups, ny)),
            dma((groups, ny)),
            dma((y_steps, groups, span, nx)),
            dma((y_steps, groups, span, nx)),
            dma((x_steps, groups, span)),
            dma((x_steps, groups, span)),
            dma((groups, span)),
            dma((nz,)),
        ],
        compiler_params=pltpu.CompilerParams(
            collective_id=0, has_side_effects=True, vmem_limit_bytes=56 * 1024 * 1024
        ),
    )(
        tokens, norm_gain.reshape(1, width), norm_bias.reshape(1, width), routes.T, route_weights.T,
        gate_w, up_w, down_w,
    )


def layout(mesh):
    experts, parts = mesh.shape["ep"], mesh.shape["tp"]
    try:
        places = mesh.devices.reshape(experts, parts)
        across = len({d.coords[0] for d in places[:, 0]})
    except AttributeError:
        across = 2
    across = across if experts % across == 0 else 1
    return experts // across, across, parts // 2, 2


def solution(mesh):
    placed = (
        P("ep", None),
        P(),
        P(),
        P("ep", None),
        P("ep", None),
        P("ep", None, "tp"),
        P("ep", None, "tp"),
        P("ep", "tp", None),
    )
    return jax.shard_map(
        functools.partial(body, layout(mesh)), mesh=mesh, in_specs=placed, out_specs=P("ep", "tp"),
        check_vma=False,
    )
```
